32 devices in a mesh: sp: 16 (over z, y, x), tp: 2 (over core).
Axes of the slice: x: 2, y: 2, z: 4, core: 2. Of those that a mesh axis runs over, the one named last changes fastest.
Arguments:
- tokens: bfloat16 [4096, 2048], P('sp', 'tp'), may hold values from -12 to 12
- norm_gain: float32 [2048], replicated, may hold values from 0.1 to 1.9
- window_query: bfloat16 [2048, 1024], P(None, 'tp'), may hold values from -2 to 2
- window_key: bfloat16 [2048, 512], P(None, 'tp'), may hold values from -2 to 2
- window_value: bfloat16 [2048, 512], P(None, 'tp'), may hold values from -0.125 to 0.125
- window_gate: bfloat16 [2048, 1024], P(None, 'tp'), may hold values from -0.125 to 0.125
- window_sink: float32 [16], P('tp'), may hold values from 2 to 6
- pair_query: bfloat16 [2048, 1024], P(None, 'tp'), may hold values from -2 to 2
- pair_key: bfloat16 [2048, 1024], P(None, 'tp'), may hold values from -2 to 2
- pair_value: bfloat16 [2048, 1024], P(None, 'tp'), may hold values from -0.125 to 0.125
- pair_gate: bfloat16 [2048, 1024], P(None, 'tp'), may hold values from -0.125 to 0.125
- map_lambda: float32 [8], P('tp'), may hold values from 0.3 to 0.8
- head_gain: float32 [128], replicated, may hold values from 0.1 to 1.9
- window_out: bfloat16 [1024, 2048], P('tp'), may hold values from -0.125 to 0.125
- pair_out: bfloat16 [1024, 2048], P('tp'), may hold values from -0.125 to 0.125
Outputs:
- mixed: bfloat16 [4096, 2048], P(('sp', 'tp'))
The draws below stay inside these ranges and needn't reach their ends.
All inputs are finite; a program needn't handle non-finite values.
Results may differ from the reference program's by a relative error of at most 0.018.
Values may be sent and summed in bfloat16 or wider, within the bound.
No kernel may reach another device: no remote copies, remote signals or barrier semaphores. Data moves between devices by JAX's collectives and lax.ppermute only.
A program may use at most 128 MiB of HBM per device.

```python
import math
import jax
import jax.numpy as jnp
from jax import lax

D = 2048
HD = 64
A_HEADS = 16
A_KV = 8
B_HEADS = 8
WINDOW = 128
SEQ = 4096
HEAD_GROUPS = 2


def base_weight(key, noise_tag, columns, fan_in):
    noise = jax.random.normal(jax.random.fold_in(key, noise_tag), (D, columns), jnp.float32)
    return jnp.clip(noise, -6.0, 6.0) * fan_in ** (-0.5)


def draw_tokens(key, part):
    values = jnp.clip(jax.random.normal(jax.random.fold_in(key, 21), (SEQ, D), jnp.float32), -6.0, 6.0)
    return values.astype(jnp.bfloat16)


def draw_window_query(key, part):
    weight = base_weight(key, 31, A_HEADS * HD, D)
    return weight.astype(jnp.bfloat16)


def draw_window_key(key, part):
    weight = base_weight(key, 32, A_KV * HD, D)
    return weight.astype(jnp.bfloat16)


def draw_pair_query(key, part):
    weight = base_weight(key, 33, B_HEADS * 2 * HD, D // 2)
    return weight.astype(jnp.bfloat16)


def draw_pair_key(key, part):
    weight = base_weight(key, 34, B_HEADS * 2 * HD, D // 2)
    return weight.astype(jnp.bfloat16)


def shard_levels(own_key, extent, pieces, least, top_value):
    def one(axis_at, parts):
        draws = jax.random.uniform(jax.random.fold_in(jax.random.fold_in(own_key, 6), axis_at), (parts,), jnp.float32, least / len(pieces), top_value / len(pieces))
        return jnp.repeat(jnp.exp(draws), extent[axis_at] // parts).reshape((-1,) + (1,) * (len(extent) - axis_at - 1))

    gain = one(*pieces[0])
    for cut in pieces[1:]:
        gain = gain * one(*cut)
    return gain


def gaussian(rng, shape, scale, bound, pieces=(), kind=jnp.bfloat16):
    loudness = shard_levels(rng, shape, pieces, -0.22, 0.18) if pieces else 1.0
    values = jax.random.normal(rng, shape, jnp.float32) * scale * loudness
    return jnp.minimum(jnp.maximum(values, -bound), bound).astype(kind)


def setup_inputs(seed: int = 0) -> dict:
    key_list = jax.random.split(jax.random.key(seed), 16)
    tokens = draw_tokens(jax.random.fold_in(key_list[15], 71), 0)
    norm_gain = jnp.clip(1.0 + 0.18 * jax.random.normal(key_list[1], (D,), jnp.float32), 0.1, 1.9)
    window_query = draw_window_query(jax.random.fold_in(key_list[15], 71), 0)
    window_key = draw_window_key(jax.random.fold_in(key_list[15], 71), 0)
    window_value = gaussian(key_list[4], (D, A_KV * HD), D ** -0.5, 0.125, ((1, 2),))
    window_gate = gaussian(key_list[5], (D, A_HEADS * HD), D ** -0.5, 0.125, ((1, 2),))
    window_sink = jnp.clip(2.0 + 4.0 * jax.random.uniform(key_list[6], (A_HEADS,), jnp.float32) ** shard_levels(key_list[6], (A_HEADS,), ((0, 2),), -0.2, 0.2), 2.0, 6.0)
    pair_query = draw_pair_query(jax.random.fold_in(key_list[15], 71), 0)
    pair_key = draw_pair_key(jax.random.fold_in(key_list[15], 71), 0)
    pair_value = gaussian(key_list[9], (D, B_HEADS * 2 * HD), D ** -0.5, 0.125, ((1, 2),))
    pair_gate = gaussian(key_list[10], (D, B_HEADS * 2 * HD), D ** -0.5, 0.125, ((1, 2),))
    map_lambda = jnp.clip(0.3 + 0.5 * jax.random.uniform(key_list[11], (B_HEADS,), jnp.float32) ** shard_levels(key_list[11], (B_HEADS,), ((0, 2),), -0.2, 0.2), 0.3, 0.8)
    head_gain = jnp.clip(1.0 + 0.18 * jax.random.normal(key_list[12], (2 * HD,), jnp.float32), 0.1, 1.9)
    window_out = gaussian(key_list[13], (A_HEADS * HD, D), (A_HEADS * HD + 2 * B_HEADS * HD) ** -0.5, 0.125, ((0, 2),))
    pair_out = gaussian(key_list[14], (2 * B_HEADS * HD, D), (A_HEADS * HD + 2 * B_HEADS * HD) ** -0.5, 0.125, ((0, 2),))
    return dict(tokens=tokens, norm_gain=norm_gain, window_query=window_query, window_key=window_key, window_value=window_value, window_gate=window_gate, window_sink=window_sink, pair_query=pair_query, pair_key=pair_key, pair_value=pair_value, pair_gate=pair_gate, map_lambda=map_lambda, head_gain=head_gain, window_out=window_out, pair_out=pair_out)


norm_eps = 1e-06
head_scale = 0.8

def row_norm(values, gain_vec):
    squares = lax.optimization_barrier(jnp.mean(values * values, axis=-1, keepdims=True))
    return values * lax.rsqrt(squares + norm_eps) * gain_vec

def reference(tokens, norm_gain, window_query, window_key, window_value, window_gate, window_sink, pair_query, pair_key, pair_value, pair_gate, map_lambda, head_gain, window_out, pair_out):
    seq_len = tokens.shape[0]
    normed = row_norm(tokens.astype(jnp.float32), norm_gain).astype(jnp.bfloat16)

    def project(weight):
        return jnp.dot(normed.astype(jnp.float32), weight.astype(jnp.float32), preferred_element_type=jnp.float32).astype(jnp.bfloat16)
    slide_query = project(window_query)
    slide_key = project(window_key)
    slide_value = project(window_value)
    slide_gate = project(window_gate)
    paired_query = project(pair_query)
    paired_key = project(pair_key)
    paired_value = project(pair_value)
    paired_gate = project(pair_gate)
    scale = HD ** (-0.5)
    group_size = A_HEADS // A_KV
    blocks_count = seq_len // WINDOW
    queries = slide_query.reshape(blocks_count, WINDOW, A_KV, group_size, HD).astype(jnp.float32)

    def band(values):
        before = jnp.pad(values, ((WINDOW, 0), (0, 0)))[:seq_len]
        return jnp.concatenate([before.reshape(blocks_count, WINDOW, A_KV, HD), values.reshape(blocks_count, WINDOW, A_KV, HD)], axis=1).astype(jnp.float32)
    band_keys = band(slide_key)
    band_values = band(slide_value)
    sink_logit = window_sink.reshape(A_KV, group_size)[:, :, None, None]
    query_idx = jnp.arange(WINDOW, dtype=jnp.int32)[:, None]
    key_idx = jnp.arange(2 * WINDOW, dtype=jnp.int32)[None, :]
    distance = query_idx - key_idx + WINDOW

    def window_block(inputs):
        block_query, block_keys, block_values, block_number = inputs
        scores = jnp.einsum('ikgd,jkd->kgij', block_query, block_keys) * scale
        valid = (distance >= 0) & (distance < WINDOW) & (block_number * WINDOW - WINDOW + key_idx >= 0)
        masked = jnp.where(valid, scores, -jnp.inf)
        top = jnp.maximum(lax.optimization_barrier(jnp.max(masked, axis=-1, keepdims=True)), sink_logit)
        weights = jnp.where(valid, jnp.exp(masked - top), 0.0)
        probs = weights / (lax.optimization_barrier(jnp.sum(weights, axis=-1, keepdims=True)) + jnp.exp(sink_logit - top))
        probs = lax.optimization_barrier(probs.astype(jnp.bfloat16)).astype(jnp.float32)
        return jnp.einsum('kgij,jkd->ikgd', probs, block_values)
    slide_out = lax.map(window_block, (queries, band_keys, band_values, jnp.arange(blocks_count, dtype=jnp.int32)))
    slide_out = slide_out.reshape(seq_len, A_HEADS * HD)
    slide_mix = (slide_out * jax.nn.silu(slide_gate.astype(jnp.float32))).astype(jnp.bfloat16)
    q_block = math.gcd(seq_len, 256)
    pair_queries = paired_query.reshape(seq_len, B_HEADS, 2, HD).astype(jnp.float32)
    pair_keys = paired_key.reshape(seq_len, B_HEADS, 2, HD).astype(jnp.float32)
    pair_values = paired_value.reshape(seq_len, B_HEADS, 2 * HD).astype(jnp.float32)
    key_pos = jnp.arange(seq_len, dtype=jnp.int32)

    def pair_block(block_number):
        begin = block_number * q_block
        block_query = lax.dynamic_slice_in_dim(pair_queries, begin, q_block, 0)
        query_pos = begin + jnp.arange(q_block, dtype=jnp.int32)
        scores = jnp.einsum('ihcd,jhcd->hcij', block_query, pair_keys) * scale
        causal = query_pos[:, None] >= key_pos[None, :]
        masked = jnp.where(causal, scores, -jnp.inf)
        top = lax.optimization_barrier(jnp.max(masked, axis=-1, keepdims=True))
        weights = jnp.where(causal, jnp.exp(masked - top), 0.0)
        totals = lax.optimization_barrier(jnp.sum(weights, axis=-1))
        rounded = lax.optimization_barrier(weights.astype(jnp.bfloat16)).astype(jnp.float32)
        numer = jnp.einsum('hcij,jhe->hcie', rounded, pair_values)
        return numer / totals[..., None]
    per_map = lax.map(pair_block, jnp.arange(seq_len // q_block, dtype=jnp.int32))
    differ = per_map[:, :, 0] - map_lambda[None, :, None, None] * per_map[:, :, 1]
    head_out = row_norm(differ, head_gain) * head_scale
    head_out = jnp.transpose(head_out, (0, 2, 1, 3)).reshape(seq_len, B_HEADS, 2 * HD)
    gate_act = jax.nn.silu(paired_gate.astype(jnp.float32).reshape(seq_len, B_HEADS, 2 * HD))
    paired_mix = (head_out * gate_act).reshape(seq_len, B_HEADS * 2 * HD).astype(jnp.bfloat16)
    slide_cols = A_HEADS * HD // HEAD_GROUPS
    paired_cols = B_HEADS * 2 * HD // HEAD_GROUPS
    total = jnp.zeros((seq_len, D), jnp.float32)
    for group_index in range(HEAD_GROUPS):
        slide_part = slide_mix[:, group_index * slide_cols:(group_index + 1) * slide_cols]
        paired_part = paired_mix[:, group_index * paired_cols:(group_index + 1) * paired_cols]
        partial_sum = jnp.dot(slide_part.astype(jnp.float32), window_out[group_index * slide_cols:(group_index + 1) * slide_cols].astype(jnp.float32), preferred_element_type=jnp.float32)
        partial_sum = partial_sum + jnp.dot(paired_part.astype(jnp.float32), pair_out[group_index * paired_cols:(group_index + 1) * paired_cols].astype(jnp.float32), preferred_element_type=jnp.float32)
        total = total + lax.optimization_barrier(partial_sum.astype(jnp.bfloat16)).astype(jnp.float32)
    return total.astype(jnp.bfloat16)
```

```python
import functools

import jax
import jax.numpy as jnp
from jax import lax
from jax.experimental import pallas as pl
from jax.experimental.pallas import tpu as pltpu
from jax.sharding import PartitionSpec as P

HD = 64
WINDOW = 128
PAIR = 2 * HD
GROUP = 4
LOW = -1e30

norm_eps = 1e-06
head_scale = 0.8


def shifted(value, axis, steps):
    count = lax.axis_size(axis)
    initial, last = (max(0, -steps), min(count, count - steps))
    return lax.ppermute(value, axis, [(source, source + steps) for source in range(initial, last)])


def exchanged(value, axis, mask):
    return lax.ppermute(value, axis, [(s, s ^ mask) for s in range(lax.axis_size(axis))])


def row_norm(values, gain_vec):
    squares = jnp.mean(values * values, axis=-1, keepdims=True)
    return values * lax.rsqrt(squares + norm_eps) * gain_vec


def pair_kernel(info_ref, lam_ref, gain_ref, q_ref, *refs, listed, pieces):
    out_ref = refs[-1]
    count = (len(refs) - 1) // 2
    key_refs, value_refs = refs[:count], refs[count:-1]
    rows = q_ref.shape[1]
    place = info_ref[0]
    block = pl.program_id(0)
    width = GROUP if not listed else count
    groups = pieces // width
    q = q_ref[0] * jnp.bfloat16(HD ** (-0.5))
    lane = lax.broadcasted_iota(jnp.int32, q.shape, 1)
    zero = jnp.zeros_like(q)
    both = jnp.concatenate([jnp.where(lane < HD, q, zero), jnp.where(lane >= HD, q, zero)], axis=0)

    def one_step(at, group, carried, masked):
        top, total, acc = carried
        if listed:
            keys = [ref[at] for ref in key_refs]
            values = [ref[at] for ref in value_refs]
            homes = [place ^ d for d in range(width)]
        else:
            keys = [key_refs[0][group * width + d, at] for d in range(width)]
            values = [value_refs[0][group * width + d, at] for d in range(width)]
            homes = [group * width + d for d in range(width)]
        scores = []
        for key_rows, home in zip(keys, homes):
            part = lax.dot_general(
                both, key_rows, (((1,), (1,)), ((), ())), preferred_element_type=jnp.float32
            )
            if masked:
                own = lax.broadcasted_iota(jnp.int32, (rows, rows), 0)
                theirs = lax.broadcasted_iota(jnp.int32, (rows, rows), 1)
                seen = own - theirs >= (home - place) * rows
                seen = jnp.concatenate([seen, seen], axis=0)
                part = jnp.where(seen, part, LOW)
            scores.append(part)
        new_top = top
        for part in scores:
            new_top = jnp.maximum(new_top, jnp.max(part, axis=-1, keepdims=True))
        factor = jnp.exp(top - new_top)
        total = total * factor
        acc = acc * factor
        for part, value_rows in zip(scores, values):
            weights = jnp.exp(part - new_top)
            total = total + jnp.sum(weights, axis=-1, keepdims=True)
            acc = acc + jnp.dot(
                weights.astype(jnp.bfloat16), value_rows, preferred_element_type=jnp.float32
            )
        return new_top, total, acc

    state = (
        jnp.full((2 * rows, 1), LOW, jnp.float32),
        jnp.zeros((2 * rows, 1), jnp.float32),
        jnp.zeros((2 * rows, PAIR), jnp.float32),
    )

    def earlier(turn, carried):
        return one_step(turn // groups, turn % groups, carried, False)

    def current(turn, carried):
        return one_step(block, turn, carried, True)

    if groups == 1:
        state = lax.fori_loop(0, block, lambda t, s: one_step(t, 0, s, False), state)
        state = one_step(block, 0, state, True)
    else:
        state = lax.fori_loop(0, block * groups, earlier, state)
        state = lax.fori_loop(0, groups, current, state)
    _, total, acc = state
    per_map = acc / total
    differ = per_map[:rows] - lam_ref[0] * per_map[rows:]
    out_ref[0] = (row_norm(differ, gain_ref[...]) * head_scale).astype(jnp.bfloat16)


def pair_attention(place, lam, gain, queries, key_list, value_list, listed, pieces):
    blocks, rows, _ = queries.shape
    whole = lambda arr: pl.BlockSpec(arr.shape, lambda i: (0,) * arr.ndim)
    smem = pl.BlockSpec(memory_space=pltpu.SMEM)
    gain = gain.reshape(1, PAIR)
    return pl.pallas_call(
        functools.partial(pair_kernel, listed=listed, pieces=pieces),
        grid=(blocks,),
        in_specs=[smem, smem, whole(gain), pl.BlockSpec((1, rows, PAIR), lambda i: (i, 0, 0))]
        + [whole(arr) for arr in key_list + value_list],
        out_specs=pl.BlockSpec((1, rows, PAIR), lambda i: (i, 0, 0)),
        out_shape=jax.ShapeDtypeStruct(queries.shape, jnp.bfloat16),
        compiler_params=pltpu.CompilerParams(vmem_limit_bytes=48 * 1024 * 1024),
        name="pair_attention",
    )(place.reshape(1), lam.reshape(1), gain, queries, *key_list, *value_list)


def per_device(
    tokens,
    norm_gain,
    window_query,
    window_key,
    window_value,
    window_gate,
    window_sink,
    pair_query,
    pair_key,
    pair_value,
    pair_gate,
    map_lambda,
    head_gain,
    window_out,
    pair_out,
):
    tok_rows = tokens.shape[0]
    tp_size = lax.axis_size("tp")
    sp_size = lax.axis_size("sp")
    core = lax.axis_index("tp")
    spot = lax.axis_index("sp")
    if tp_size == 2:
        other = exchanged(tokens, "tp", 1)
        gathered = jnp.concatenate(
            [jnp.where(core == 0, tokens, other), jnp.where(core == 0, other, tokens)], axis=1
        )
    else:
        gathered = lax.all_gather(tokens, "tp", axis=1, tiled=True)
    normed = row_norm(gathered.astype(jnp.float32), norm_gain).astype(jnp.bfloat16)

    def project(weight):
        return jnp.dot(normed, weight, preferred_element_type=jnp.float32).astype(jnp.bfloat16)

    heads = pair_query.shape[1] // PAIR
    stride = sp_size // heads
    share = spot // stride
    place = spot % stride

    def head_columns(value, head):
        return lax.dynamic_slice_in_dim(value, head * PAIR, PAIR, 1)

    def by_share(received):
        if heads == 1:
            return received[0][None]
        stacked = jnp.stack(received)
        return jnp.stack(
            [lax.dynamic_index_in_dim(stacked, share ^ j, 0, keepdims=False) for j in range(heads)]
        )

    def to_heads(*values):
        width = len(values) * PAIR
        received = []
        for d in range(heads):
            piece = jnp.concatenate([head_columns(v, share ^ d) for v in values], axis=1)
            received.append(exchanged(piece, "sp", d * stride) if d else piece)
        return [
            by_share([piece[:, i * PAIR : (i + 1) * PAIR] for piece in received])
            for i in range(len(values))
        ]

    listed = stride <= GROUP

    def gather_places(value):
        if listed:
            return [exchanged(value, "sp", d) if d else value for d in range(stride)]
        named = [[s * stride + p for p in range(stride)] for s in range(heads)]
        return [lax.all_gather(value, "sp", axis=0, axis_index_groups=named)]

    (key_rows,) = to_heads(project(pair_key))
    key_list = gather_places(key_rows)
    value_rows, query_rows = to_heads(project(pair_value), project(pair_query))
    value_list = gather_places(value_rows)

    slide_key = project(window_key)
    slide_value = project(window_value)
    tails = shifted(
        jnp.concatenate([slide_key[tok_rows - WINDOW :], slide_value[tok_rows - WINDOW :]], axis=1),
        "sp",
        1,
    )
    tail_keys, tail_values = jnp.split(tails, 2, axis=1)
    slide_query = project(window_query)
    slide_gate = project(window_gate)
    paired_gate = project(pair_gate)
    scale = HD ** (-0.5)
    kv_heads = slide_key.shape[1] // HD
    group_size = slide_query.shape[1] // slide_key.shape[1]
    offset = spot * tok_rows
    query_pos = offset + jnp.arange(tok_rows, dtype=jnp.int32)
    band_keys = jnp.concatenate([tail_keys, slide_key], axis=0).reshape(
        WINDOW + tok_rows, kv_heads, HD
    )
    band_values = jnp.concatenate([tail_values, slide_value], axis=0).reshape(
        WINDOW + tok_rows, kv_heads, HD
    )
    band_pos = offset - WINDOW + jnp.arange(WINDOW + tok_rows, dtype=jnp.int32)
    window_queries = slide_query.reshape(tok_rows, kv_heads, group_size, HD)
    scores = (
        jnp.einsum("ikgd,jkd->kgij", window_queries, band_keys, preferred_element_type=jnp.float32)
        * scale
    )
    distance = query_pos[:, None] - band_pos[None, :]
    valid = (distance >= 0) & (distance < WINDOW) & (band_pos[None, :] >= 0)
    masked = jnp.where(valid, scores, -jnp.inf)
    sink_logit = window_sink.reshape(kv_heads, group_size)[:, :, None, None]
    top = jnp.maximum(jnp.max(masked, axis=-1, keepdims=True), sink_logit)
    weights = jnp.where(valid, jnp.exp(masked - top), 0.0)
    probs = (
        weights / (jnp.sum(weights, axis=-1, keepdims=True) + jnp.exp(sink_logit - top))
    ).astype(jnp.bfloat16)
    slide_out = jnp.einsum("kgij,jkd->ikgd", probs, band_values, preferred_element_type=jnp.float32)
    slide_out = slide_out.reshape(tok_rows, kv_heads * group_size * HD)
    slide_mix = (slide_out * jax.nn.silu(slide_gate.astype(jnp.float32))).astype(jnp.bfloat16)
    slide_part = jnp.dot(slide_mix, window_out, preferred_element_type=jnp.float32)
    gate_act = jax.nn.silu(paired_gate.astype(jnp.float32))
    mine = lax.dynamic_index_in_dim(map_lambda, share, 0, keepdims=False)
    found = pair_attention(
        place, mine, head_gain, query_rows, key_list, value_list, listed, stride
    )
    returned = []
    for d in range(heads):
        piece = lax.dynamic_index_in_dim(found, share ^ d, 0, keepdims=False)
        returned.append(exchanged(piece, "sp", d * stride) if d else piece)
    head_out = jnp.concatenate(list(by_share(returned)), axis=1)
    paired_mix = (head_out.astype(jnp.float32) * gate_act).astype(jnp.bfloat16)

    def partial_rows(begin, count):
        mix = lax.dynamic_slice_in_dim(paired_mix, begin, count, 0)
        part = jnp.dot(mix, pair_out, preferred_element_type=jnp.float32)
        part = part + lax.dynamic_slice_in_dim(slide_part, begin, count, 0)
        return lax.optimization_barrier(part.astype(jnp.bfloat16))

    if tp_size == 2:
        half = tok_rows // 2
        theirs = exchanged(partial_rows((1 - core) * half, half), "tp", 1)
        ours = partial_rows(core * half, half)
        return (ours.astype(jnp.float32) + theirs.astype(jnp.float32)).astype(jnp.bfloat16)
    return lax.psum_scatter(
        partial_rows(0, tok_rows), "tp", scatter_dimension=0, tiled=True
    )


def solution(mesh):
    in_specs = (
        P("sp", "tp"),
        P(),
        P(None, "tp"),
        P(None, "tp"),
        P(None, "tp"),
        P(None, "tp"),
        P("tp"),
        P(None, "tp"),
        P(None, "tp"),
        P(None, "tp"),
        P(None, "tp"),
        P("tp"),
        P(),
        P("tp", None),
        P("tp", None),
    )
    out_specs = P(("sp", "tp"), None)
    return jax.shard_map(
        per_device, mesh=mesh, in_specs=in_specs, out_specs=out_specs, check_vma=False
    )
```

```python
import functools

import jax
import jax.numpy as jnp
from jax import lax
from jax.experimental import pallas as pl
from jax.experimental.pallas import tpu as pltpu
from jax.sharding import PartitionSpec as P

HD = 64
WINDOW = 128
PAIR = 2 * HD
GROUP = 4
LOW = -1e30

norm_eps = 1e-06
head_scale = 0.8


def shifted(value, axis, steps):
    count = lax.axis_size(axis)
    initial, last = (max(0, -steps), min(count, count - steps))
    return lax.ppermute(value, axis, [(source, source + steps) for source in range(initial, last)])


def exchanged(value, axis, mask):
    return lax.ppermute(value, axis, [(s, s ^ mask) for s in range(lax.axis_size(axis))])


def row_norm(values, gain_vec):
    squares = jnp.mean(values * values, axis=-1, keepdims=True)
    return values * lax.rsqrt(squares + norm_eps) * gain_vec


def pair_kernel(info_ref, lam_ref, gain_ref, q_ref, *refs, listed, pieces):
    out_ref = refs[-1]
    count = (len(refs) - 1) // 2
    key_refs, value_refs = refs[:count], refs[count:-1]
    rows = q_ref.shape[1]
    place = info_ref[0]
    block = pl.program_id(0)
    width = GROUP if not listed else count
    groups = pieces // width
    q = q_ref[0] * jnp.bfloat16(HD ** (-0.5))
    lane = lax.broadcasted_iota(jnp.int32, q.shape, 1)
    zero = jnp.zeros_like(q)
    both = jnp.concatenate([jnp.where(lane < HD, q, zero), jnp.where(lane >= HD, q, zero)], axis=0)

    def one_step(at, group, carried, masked):
        top, total, acc = carried
        if listed:
            keys = [ref[at] for ref in key_refs]
            values = [ref[at] for ref in value_refs]
            homes = [place ^ d for d in range(width)]
        else:
            keys = [key_refs[0][group * width + d, at] for d in range(width)]
            values = [value_refs[0][group * width + d, at] for d in range(width)]
            homes = [group * width + d for d in range(width)]
        scores = lax.dot_general(
            both,
            jnp.concatenate(keys, axis=0),
            (((1,), (1,)), ((), ())),
            preferred_element_type=jnp.float32,
        )
        if masked:
            own = lax.broadcasted_iota(jnp.int32, (rows, rows), 0)
            theirs = lax.broadcasted_iota(jnp.int32, (rows, rows), 1)
            gap = own - theirs
            seen = jnp.concatenate([gap >= (home - place) * rows for home in homes], axis=1)
            scores = jnp.where(jnp.concatenate([seen, seen], axis=0), scores, LOW)
        new_top = jnp.maximum(top, jnp.max(scores, axis=-1, keepdims=True))
        factor = jnp.exp(top - new_top)
        weights = jnp.exp(scores - new_top)
        total = total * factor
        for begin in range(0, width * rows, 128):
            total = total + weights[:, begin : begin + 128]
        acc = acc * factor + jnp.dot(
            weights.astype(jnp.bfloat16),
            jnp.concatenate(values, axis=0),
            preferred_element_type=jnp.float32,
        )
        return new_top, total, acc

    state = (
        jnp.full((2 * rows, 1), LOW, jnp.float32),
        jnp.zeros((2 * rows, 128), jnp.float32),
        jnp.zeros((2 * rows, PAIR), jnp.float32),
    )

    def earlier(turn, carried):
        return one_step(turn // groups, turn % groups, carried, False)

    def current(turn, carried):
        return one_step(block, turn, carried, True)

    if groups == 1:
        state = lax.fori_loop(0, block, lambda t, s: one_step(t, 0, s, False), state)
        state = one_step(block, 0, state, True)
    else:
        state = lax.fori_loop(0, block * groups, earlier, state)
        state = lax.fori_loop(0, groups, current, state)
    _, total, acc = state
    per_map = acc / jnp.sum(total, axis=-1, keepdims=True)
    differ = per_map[:rows] - lam_ref[0] * per_map[rows:]
    out_ref[0] = (row_norm(differ, gain_ref[...]) * head_scale).astype(jnp.bfloat16)


def pair_attention(place, lam, gain, queries, key_list, value_list, listed, pieces):
    blocks, rows, _ = queries.shape
    whole = lambda arr: pl.BlockSpec(arr.shape, lambda i: (0,) * arr.ndim)
    smem = pl.BlockSpec(memory_space=pltpu.SMEM)
    gain = gain.reshape(1, PAIR)
    return pl.pallas_call(
        functools.partial(pair_kernel, listed=listed, pieces=pieces),
        grid=(blocks,),
        in_specs=[smem, smem, whole(gain), pl.BlockSpec((1, rows, PAIR), lambda i: (i, 0, 0))]
        + [whole(arr) for arr in key_list + value_list],
        out_specs=pl.BlockSpec((1, rows, PAIR), lambda i: (i, 0, 0)),
        out_shape=jax.ShapeDtypeStruct(queries.shape, jnp.bfloat16),
        compiler_params=pltpu.CompilerParams(vmem_limit_bytes=48 * 1024 * 1024),
        name="pair_attention",
    )(place.reshape(1), lam.reshape(1), gain, queries, *key_list, *value_list)


def per_device(
    tokens,
    norm_gain,
    window_query,
    window_key,
    window_value,
    window_gate,
    window_sink,
    pair_query,
    pair_key,
    pair_value,
    pair_gate,
    map_lambda,
    head_gain,
    window_out,
    pair_out,
):
    tok_rows = tokens.shape[0]
    tp_size = lax.axis_size("tp")
    sp_size = lax.axis_size("sp")
    core = lax.axis_index("tp")
    spot = lax.axis_index("sp")
    if tp_size == 2:
        other = exchanged(tokens, "tp", 1)
        gathered = jnp.concatenate(
            [jnp.where(core == 0, tokens, other), jnp.where(core == 0, other, tokens)], axis=1
        )
    else:
        gathered = lax.all_gather(tokens, "tp", axis=1, tiled=True)
    normed = row_norm(gathered.astype(jnp.float32), norm_gain).astype(jnp.bfloat16)

    def project(weight):
        return jnp.dot(normed, weight, preferred_element_type=jnp.float32).astype(jnp.bfloat16)

    heads = pair_query.shape[1] // PAIR
    stride = sp_size // heads
    share = spot // stride
    place = spot % stride

    def head_columns(value, head):
        return lax.dynamic_slice_in_dim(value, head * PAIR, PAIR, 1)

    def by_share(received):
        if heads == 1:
            return received[0][None]
        stacked = jnp.stack(received)
        return jnp.stack(
            [lax.dynamic_index_in_dim(stacked, share ^ j, 0, keepdims=False) for j in range(heads)]
        )

    def to_heads(*values):
        width = len(values) * PAIR
        received = []
        for d in range(heads):
            piece = jnp.concatenate([head_columns(v, share ^ d) for v in values], axis=1)
            received.append(exchanged(piece, "sp", d * stride) if d else piece)
        return [
            by_share([piece[:, i * PAIR : (i + 1) * PAIR] for piece in received])
            for i in range(len(values))
        ]

    listed = stride <= GROUP

    def gather_places(value):
        if listed:
            return [exchanged(value, "sp", d) if d else value for d in range(stride)]
        named = [[s * stride + p for p in range(stride)] for s in range(heads)]
        return [lax.all_gather(value, "sp", axis=0, axis_index_groups=named)]

    (key_rows,) = to_heads(project(pair_key))
    key_list = gather_places(key_rows)
    value_rows, query_rows = to_heads(project(pair_value), project(pair_query))
    value_list = gather_places(value_rows)

    slide_key = project(window_key)
    slide_value = project(window_value)
    tails = shifted(
        jnp.concatenate([slide_key[tok_rows - WINDOW :], slide_value[tok_rows - WINDOW :]], axis=1),
        "sp",
        1,
    )
    tail_keys, tail_values = jnp.split(tails, 2, axis=1)
    slide_query = project(window_query)
    slide_gate = project(window_gate)
    paired_gate = project(pair_gate)
    scale = HD ** (-0.5)
    kv_heads = slide_key.shape[1] // HD
    group_size = slide_query.shape[1] // slide_key.shape[1]
    offset = spot * tok_rows
    query_pos = offset + jnp.arange(tok_rows, dtype=jnp.int32)
    band_keys = jnp.concatenate([tail_keys, slide_key], axis=0).reshape(
        WINDOW + tok_rows, kv_heads, HD
    )
    band_values = jnp.concatenate([tail_values, slide_value], axis=0).reshape(
        WINDOW + tok_rows, kv_heads, HD
    )
    band_pos = offset - WINDOW + jnp.arange(WINDOW + tok_rows, dtype=jnp.int32)
    window_queries = slide_query.reshape(tok_rows, kv_heads, group_size, HD)
    scores = (
        jnp.einsum("ikgd,jkd->kgij", window_queries, band_keys, preferred_element_type=jnp.float32)
        * scale
    )
    distance = query_pos[:, None] - band_pos[None, :]
    valid = (distance >= 0) & (distance < WINDOW) & (band_pos[None, :] >= 0)
    masked = jnp.where(valid, scores, -jnp.inf)
    sink_logit = window_sink.reshape(kv_heads, group_size)[:, :, None, None]
    top = jnp.maximum(jnp.max(masked, axis=-1, keepdims=True), sink_logit)
    weights = jnp.where(valid, jnp.exp(masked - top), 0.0)
    probs = (
        weights / (jnp.sum(weights, axis=-1, keepdims=True) + jnp.exp(sink_logit - top))
    ).astype(jnp.bfloat16)
    slide_out = jnp.einsum("kgij,jkd->ikgd", probs, band_values, preferred_element_type=jnp.float32)
    slide_out = slide_out.reshape(tok_rows, kv_heads * group_size * HD)
    slide_mix = (slide_out * jax.nn.silu(slide_gate.astype(jnp.float32))).astype(jnp.bfloat16)
    slide_part = jnp.dot(slide_mix, window_out, preferred_element_type=jnp.float32)
    gate_act = jax.nn.silu(paired_gate.astype(jnp.float32))
    mine = lax.dynamic_index_in_dim(map_lambda, share, 0, keepdims=False)
    found = pair_attention(
        place, mine, head_gain, query_rows, key_list, value_list, listed, stride
    )
    returned = []
    for d in range(heads):
        piece = lax.dynamic_index_in_dim(found, share ^ d, 0, keepdims=False)
        returned.append(exchanged(piece, "sp", d * stride) if d else piece)
    head_out = jnp.concatenate(list(by_share(returned)), axis=1)
    paired_mix = (head_out.astype(jnp.float32) * gate_act).astype(jnp.bfloat16)

    def partial_rows(begin, count):
        mix = lax.dynamic_slice_in_dim(paired_mix, begin, count, 0)
        part = jnp.dot(mix, pair_out, preferred_element_type=jnp.float32)
        part = part + lax.dynamic_slice_in_dim(slide_part, begin, count, 0)
        return lax.optimization_barrier(part.astype(jnp.bfloat16))

    if tp_size == 2:
        half = tok_rows // 2
        theirs = exchanged(partial_rows((1 - core) * half, half), "tp", 1)
        ours = partial_rows(core * half, half)
        return (ours.astype(jnp.float32) + theirs.astype(jnp.float32)).astype(jnp.bfloat16)
    return lax.psum_scatter(
        partial_rows(0, tok_rows), "tp", scatter_dimension=0, tiled=True
    )


def solution(mesh):
    in_specs = (
        P("sp", "tp"),
        P(),
        P(None, "tp"),
        P(None, "tp"),
        P(None, "tp"),
        P(None, "tp"),
        P("tp"),
        P(None, "tp"),
        P(None, "tp"),
        P(None, "tp"),
        P(None, "tp"),
        P("tp"),
        P(),
        P("tp", None),
        P("tp", None),
    )
    out_specs = P(("sp", "tp"), None)
    return jax.shard_map(
        per_device, mesh=mesh, in_specs=in_specs, out_specs=out_specs, check_vma=False
    )
```
